32 devices in a mesh: ep: 32 (over z, y, x, core).
Axes of the slice: x: 2, y: 2, z: 4, core: 2. Of those that a mesh axis runs over, the one named last changes fastest.
Arguments:
- tokens: bfloat16 [512, 2048], P('ep'), may hold values from -6 to 6
- hidden_state: float32 [512, 1024], P('ep'), may hold values from -3 to 3
- recent_inputs: bfloat16 [512, 3, 1024], P('ep'), may hold values from -6 to 6
- routes: int32 [512, 2], P('ep'), may hold values from 0 to 7, all different within a row; in each aligned block of 16 rows (0 to 15, 16 to 31, ...) at most 8 rows name the same one
- gain_mix: bfloat16 [2048], replicated, may hold values from 0.099609375 to 1.8984375
- input_weight: bfloat16 [2048, 1024], replicated, may hold values from -0.125 to 0.125
- branch_weight: bfloat16 [2048, 1024], replicated, may hold values from -0.125 to 0.125
- filter_taps: bfloat16 [4, 1024], replicated, may hold values from -3 to 3
- recurrence_map: bfloat16 [8, 128, 128], replicated, may hold values from -0.5 to 0.5
- input_map: bfloat16 [8, 128, 128], replicated, may hold values from -0.5 to 0.5
- decay_param: float32 [1024], replicated, may hold values from 0.5 to 6
- output_weight: bfloat16 [1024, 2048], replicated, may hold values from -0.1875 to 0.1875
- gain_experts: bfloat16 [2048], replicated, may hold values from 0.099609375 to 1.8984375
- router_weight: bfloat16 [2048, 8], replicated, may hold values from -0.125 to 0.125
- expert_gate: bfloat16 [2048, 32768], P(None, 'ep'), may hold values from -0.125 to 0.125
- expert_up: bfloat16 [2048, 32768], P(None, 'ep'), may hold values from -0.125 to 0.125
- expert_down: bfloat16 [32768, 2048], P('ep'), may hold values from -0.09375 to 0.09375
Outputs:
- layer_out: bfloat16 [512, 2048], P('ep')
- new_hidden: float32 [512, 1024], P('ep')
- new_inputs: bfloat16 [512, 3, 1024], P('ep')
The draws below stay inside these ranges and needn't reach their ends.
Inputs may be any that keep to these rules, and one draw needn't show every extreme that they name: `routes`: each row names 2 different experts. The rows of one device name one expert at most 8 times; in every draw some device names some expert exactly 8 times.
All inputs are finite; a program needn't handle non-finite values.
Results may differ from the reference program's by a relative error of at most 0.01.
Values may be sent and summed in bfloat16 or wider, within the bound.
A program may use at most 128 MiB of HBM per device.

```python
import math
import jax
import jax.numpy as jnp
import numpy as np
from jax import lax

D = 2048
RNN = 1024
LB = 128
NB = 8
CONV = 4
FF = 4096
EXPERTS = 8
TOP = 2
SEQ_DEV = 16
BATCH = 512
CAP = 8
N_EP = 32


def block_levels(own_key, dims, shards, low, high):
    level = 1.0
    for dim, blocks in shards:
        heights = jax.random.uniform(jax.random.fold_in(jax.random.fold_in(own_key, 6), dim), (blocks,), jnp.float32, low / len(shards), high / len(shards))
        level = level * jnp.repeat(jnp.exp(heights), dims[dim] // blocks).reshape((-1,) + (1,) * (len(dims) - 1 - dim))
    return level


def assign_block(stream_key, own, number, rows, number_of, top, limit, skew):
    ranking = jax.random.permutation(stream_key, number_of)
    heavy_load, usual = shares(number_of, rows * top, limit, skew, True), shares(number_of, rows * top, limit, skew, False)
    places = jnp.arange(number_of)

    def named(sizes, rotation):
        used = int((sizes > 0).sum())
        fixed = max(1, used // 4)
        moved = fixed + (places - fixed + rotation * (used - fixed)) % max(1, number_of - fixed)
        return jnp.zeros((number_of,), jnp.int32).at[ranking[jnp.where(places < fixed, places, moved)]].set(jnp.asarray(sizes, jnp.int32))

    sizes = jnp.where(number % 4 == 0, named(heavy_load, number // 4), named(usual, number - number // 4 - 1))
    mixed = jax.random.permutation(jax.random.fold_in(own, 3), number_of)
    giver, sink = mixed[0:number_of // 2 * 2:2], mixed[1:number_of // 2 * 2:2]
    room = jnp.minimum(sizes[giver] - 1, limit - sizes[sink]) // 2
    room = jnp.where((giver == ranking[0]) | (sink == ranking[0]) | (sizes[sink] == 0), 0, jnp.maximum(room, 0))
    moved = jax.random.randint(jax.random.fold_in(own, 4), (number_of // 2,), 0, 1 << 20) % (room + 1)
    sizes = sizes.at[giver].add(-moved).at[sink].add(moved)
    members = jnp.searchsorted(jnp.cumsum(sizes), jnp.arange(rows * top), side="right").astype(jnp.int32)
    table = members.reshape(top, rows).T
    table = table[jax.random.permutation(jax.random.fold_in(own, 1), rows)]
    rotation = jax.random.randint(jax.random.fold_in(own, 2), (rows, 1), 0, top)
    return jnp.take_along_axis(table, (jnp.arange(top)[None, :] + rotation) % top, axis=1)


def shares(amount, total, most, slope, full):
    portions = [(1 << 20) // math.isqrt(rank ** slope) + 1 for rank in range(1, amount + 1)]
    largest = most if full else min(most, max(-(-total // amount), total * portions[0] // sum(portions)))
    least = 1 if total - largest >= amount - 1 else 0
    counts, rest = [largest] + [least] * (amount - 1), total - largest - least * (amount - 1)
    while rest > 0:
        movable = [i for i in range(1, amount) if counts[i] < largest] or [i for i in range(1, amount) if counts[i] < most]
        mass, budget = sum([portions[i] for i in movable]), rest
        for i in movable:
            more = min(most - counts[i], max(1, budget * portions[i] // mass), rest)
            counts[i] = counts[i] + more
            rest = rest - more
    return np.array(counts)


def bell_draw(rng, extent, scale, bound, shards=(), kind=jnp.bfloat16):
    drawn = scale * jax.random.normal(rng, extent, jnp.float32)
    if shards:
        drawn = drawn * block_levels(rng, extent, shards, -0.22, 0.18)
    return jnp.clip(drawn, -bound, bound).astype(kind)


def setup_inputs(seed: int = 0) -> dict:
    key_of = jax.random.split(jax.random.key(seed), 18)
    tokens = bell_draw(key_of[0], (BATCH, D), 1.0, 6.0, ((0, 32),))
    hidden_state = bell_draw(key_of[1], (BATCH, RNN), 0.5, 3.0, ((0, 32),), jnp.float32)
    recent_inputs = bell_draw(key_of[2], (BATCH, CONV - 1, RNN), 1.0, 6.0, ((0, 32),))
    routes_keys = jax.random.split(jax.random.fold_in(key_of[3], 1), BATCH // SEQ_DEV)
    routes_turns = jax.random.permutation(jax.random.fold_in(key_of[3], 3), BATCH // SEQ_DEV)
    routes = jax.vmap(lambda own, number: assign_block(jax.random.fold_in(key_of[3], 2), own, number, SEQ_DEV, EXPERTS, TOP, CAP, 2))(routes_keys, routes_turns).reshape((BATCH, TOP))
    gain_mix = jnp.clip(1.0 + 0.18 * jax.random.normal(key_of[4], (D,), jnp.float32), 0.099609375, 1.8984375).astype(jnp.bfloat16)
    input_weight = bell_draw(key_of[5], (D, RNN), D ** -0.5, 0.125)
    branch_weight = bell_draw(key_of[6], (D, RNN), D ** -0.5, 0.125)
    filter_taps = bell_draw(key_of[7], (CONV, RNN), CONV ** -0.5, 3.0)
    recurrence_map = bell_draw(key_of[8], (NB, LB, LB), LB ** -0.5, 0.5)
    input_map = bell_draw(key_of[9], (NB, LB, LB), LB ** -0.5, 0.5)
    decay_param = jnp.clip(jax.random.uniform(key_of[10], (RNN,), jnp.float32, 0.5, 6.0), 0.5, 6.0)
    output_weight = bell_draw(key_of[11], (RNN, D), RNN ** -0.5, 0.1875)
    gain_experts = jnp.clip(1.0 + 0.18 * jax.random.normal(key_of[12], (D,), jnp.float32), 0.099609375, 1.8984375).astype(jnp.bfloat16)
    router_weight = bell_draw(key_of[13], (D, EXPERTS), D ** -0.5, 0.125)
    expert_gate = bell_draw(key_of[14], (D, EXPERTS * FF), D ** -0.5, 0.125, ((1, 32),))
    expert_up = bell_draw(key_of[15], (D, EXPERTS * FF), D ** -0.5, 0.125, ((1, 32),))
    expert_down = bell_draw(key_of[16], (EXPERTS * FF, D), FF ** -0.5, 0.09375, ((0, 32),))
    return dict(tokens=tokens, hidden_state=hidden_state, recent_inputs=recent_inputs, routes=routes, gain_mix=gain_mix, input_weight=input_weight, branch_weight=branch_weight, filter_taps=filter_taps, recurrence_map=recurrence_map, input_map=input_map, decay_param=decay_param, output_weight=output_weight, gain_experts=gain_experts, router_weight=router_weight, expert_gate=expert_gate, expert_up=expert_up, expert_down=expert_down)


epsilon = 1e-06
rate_scale = 8.0

def rms_scale(values, gain):
    mean_square = lax.optimization_barrier(jnp.mean(values * values, axis=-1, keepdims=True))
    return values * lax.rsqrt(mean_square + epsilon) * gain.astype(jnp.float32)

def mixer_step(tokens, hidden_state, recent_inputs, gain_mix, input_weight, branch_weight, filter_taps, recurrence_map, input_map, decay_param, output_weight):
    resid = tokens.astype(jnp.float32)
    normed = rms_scale(resid, gain_mix).astype(jnp.bfloat16)
    branch_x = jnp.dot(normed, input_weight, preferred_element_type=jnp.float32).astype(jnp.bfloat16)
    branch_g = jnp.dot(normed, branch_weight, preferred_element_type=jnp.float32).astype(jnp.bfloat16)
    window = jnp.concatenate([recent_inputs, branch_x[:, None, :]], axis=1)
    new_inputs = window[:, 1:, :]
    conv_out = lax.optimization_barrier(jnp.sum(window.astype(jnp.float32) * filter_taps.astype(jnp.float32)[None], axis=1)).astype(jnp.bfloat16)
    width = recurrence_map.shape[1]
    blocks = conv_out.reshape(conv_out.shape[0], -1, width).astype(jnp.float32)
    rec_gate = jax.nn.sigmoid(jnp.einsum('sni,nij->snj', blocks, recurrence_map.astype(jnp.float32)).reshape(conv_out.shape))
    in_gate = jax.nn.sigmoid(jnp.einsum('sni,nij->snj', blocks, input_map.astype(jnp.float32)).reshape(conv_out.shape))
    log_decay = -rate_scale * rec_gate * jax.nn.softplus(-decay_param)
    new_hidden = jnp.exp(log_decay) * hidden_state + jnp.sqrt(-jnp.expm1(2.0 * log_decay)) * (in_gate * conv_out.astype(jnp.float32))
    mixed = (new_hidden * jax.nn.gelu(branch_g.astype(jnp.float32))).astype(jnp.bfloat16)
    after = resid + jnp.dot(mixed, output_weight, preferred_element_type=jnp.float32)
    return (after, new_hidden, new_inputs)

def route_weights(normed_rows, router_weight, routes):
    logits = jnp.dot(normed_rows, router_weight, preferred_element_type=jnp.float32)
    expert_ids = jnp.arange(router_weight.shape[1], dtype=jnp.int32)
    picks = routes[:, :, None] == expert_ids[None, None, :]
    chosen = lax.optimization_barrier(jnp.sum(jnp.where(picks, logits[:, None, :], jnp.float32(0.0)), axis=-1))
    spread = chosen[:, 0] - chosen[:, 1]
    share = jnp.stack([jax.nn.sigmoid(spread), jax.nn.sigmoid(-spread)], axis=1)
    return lax.optimization_barrier(jnp.sum(jnp.where(picks, share[:, :, None], jnp.float32(0.0)), axis=1))

def slot_table(route_blocks, expert_ids, capacity):
    member = jnp.any(route_blocks[:, :, :, None] == expert_ids[None, None, None, :], axis=2)
    order = jnp.cumsum(member.astype(jnp.int32), axis=1) - 1
    slot_ids = jnp.arange(capacity, dtype=jnp.int32)
    return (member[..., None] & (order[..., None] == slot_ids)).astype(jnp.float32)

def expert_rows(packed, gate_cols, up_cols, down_rows):
    gate = jnp.dot(packed, gate_cols, preferred_element_type=jnp.float32)
    upper = jnp.dot(packed, up_cols, preferred_element_type=jnp.float32)
    inner = (jax.nn.silu(gate) * upper).astype(jnp.bfloat16)
    return jnp.dot(inner, down_rows, preferred_element_type=jnp.float32)

def reference(tokens, hidden_state, recent_inputs, routes, gain_mix, input_weight, branch_weight, filter_taps, recurrence_map, input_map, decay_param, output_weight, gain_experts, router_weight, expert_gate, expert_up, expert_down):
    after, new_hidden, new_inputs = mixer_step(tokens, hidden_state, recent_inputs, gain_mix, input_weight, branch_weight, filter_taps, recurrence_map, input_map, decay_param, output_weight)
    expert_in = rms_scale(after, gain_experts).astype(jnp.bfloat16)
    weight_table = route_weights(expert_in, router_weight, routes)
    row_blocks = expert_in.reshape(N_EP, SEQ_DEV, D).astype(jnp.float32)
    route_blocks = routes.reshape(N_EP, SEQ_DEV, TOP)
    weight_blocks = weight_table.reshape(N_EP, SEQ_DEV, EXPERTS)
    total = jnp.zeros((N_EP, SEQ_DEV, D), jnp.float32)
    for expert in range(EXPERTS):
        table = slot_table(route_blocks, jnp.array([expert], jnp.int32), CAP)[:, :, 0, :]
        packed = jnp.einsum('nsc,nsd->ncd', table, row_blocks).astype(jnp.bfloat16)
        lower = expert * FF
        result = expert_rows(packed.reshape(-1, D), expert_gate[:, lower:lower + FF], expert_up[:, lower:lower + FF], expert_down[lower:lower + FF, :])
        result = result.reshape(N_EP, CAP, D)
        scaled = table * weight_blocks[:, :, expert, None]
        total = total + jnp.einsum('nsc,ncd->nsd', scaled, result, precision=lax.Precision.HIGHEST)
    layer_out = (after + total.reshape(-1, D)).astype(jnp.bfloat16)
    return (layer_out, new_hidden, new_inputs)
```

```python
import functools

import jax
import jax.numpy as jnp
from jax import lax
from jax.experimental import pallas as pl
from jax.experimental.pallas import tpu as pltpu
from jax.sharding import PartitionSpec as P

EXPERTS = 8
CAP = 8
TAPS = 4
BITS = 3
ORDER = (1, 4, 6, 2, 5, 7, 3)

epsilon = 1e-06
rate_scale = 8.0

f32 = jnp.float32
bf16 = jnp.bfloat16


def rms_scale(values, gain):
    mean_square = jnp.mean(values * values, axis=-1, keepdims=True)
    return values * lax.rsqrt(mean_square + epsilon) * gain.astype(f32)


def flip(e, k):
    out = 0
    for i in range(BITS):
        bit = (e // (1 << i)) % 2
        if (k >> i) & 1:
            bit = 1 - bit
        out = out + bit * (1 << i)
    return out


def kernel(
    n,
    n_col,
    tokens,
    hidden_state,
    recent,
    routes,
    gain_mix,
    filter_taps,
    recurrence_map,
    input_map,
    decay_param,
    gain_experts,
    router_weight,
    w_in_hbm,
    w_branch_hbm,
    w_out_hbm,
    w_gate_hbm,
    w_up_hbm,
    w_down_hbm,
    layer_out,
    new_hidden_out,
    branch_out,
    w_in,
    w_branch,
    w_out,
    w_gate,
    w_up,
    w_down,
    after_ref,
    packed,
    x_blocks,
    x_rows,
    inner,
    a_send,
    a_recv,
    keep,
    b_send,
    b_recv,
    keep_own,
    c_send,
    c_recv,
    w_sem,
    d1_s,
    d1_r,
    d2_s,
    d2_r,
    d3_s,
    d3_r,
    a_s,
    a_r,
    b_s,
    b_r,
    c_s,
    c_r,
):
    me = lax.axis_index("ep")
    group = n // EXPERTS
    chips = group // 2
    e = me // group
    q = me % group
    core = me % 2
    chip = q // 2
    partner = me + 1 - 2 * core

    def peer_chip(d):
        return e * group + ((chip + d) % chips) * 2 + core

    def remote(src, dst, ssem, rsem, dev):
        return pltpu.make_async_remote_copy(
            src_ref=src,
            dst_ref=dst,
            send_sem=ssem,
            recv_sem=rsem,
            device_id=(dev,),
            device_id_type=pl.DeviceIdType.MESH,
        )

    barrier = pltpu.get_barrier_semaphore()
    peers = [flip(e, k) * group + q for k in range(1, EXPERTS)]
    peers += [partner] + [peer_chip(d) for d in range(1, chips)]
    for dev in peers:
        pl.semaphore_signal(
            barrier, inc=1, device_id=(dev,), device_id_type=pl.DeviceIdType.MESH
        )

    parts = 4
    loads = []

    def load(src, dst, pieces):
        rows = src.shape[0] // pieces
        made = []
        for i in range(pieces):
            cut = pl.ds(i * rows, rows)
            made.append(pltpu.make_async_copy(src.at[cut], dst.at[cut], w_sem.at[len(loads)]))
            loads.append(made[-1])
        return made

    in_loads = load(w_in_hbm, w_in, parts)
    branch_loads = load(w_branch_hbm, w_branch, parts)
    out_loads = load(w_out_hbm, w_out, parts)
    expert_loads = load(w_gate_hbm, w_gate, 1) + load(w_up_hbm, w_up, 1) + load(w_down_hbm, w_down, 1)
    for copy in loads:
        copy.start()

    def streamed(lhs, weight, copies):
        rows = weight.shape[0] // len(copies)
        total = None
        for i, copy in enumerate(copies):
            copy.wait()
            part = jnp.dot(
                lhs[:, i * rows : (i + 1) * rows],
                weight[i * rows : (i + 1) * rows, :],
                preferred_element_type=f32,
            )
            total = part if total is None else total + part
        return total

    resid = tokens[...].astype(f32)
    normed = rms_scale(resid, gain_mix[...]).astype(bf16)
    branch_x = streamed(normed, w_in, in_loads).astype(bf16)
    branch_out[...] = branch_x
    rnn = branch_x.shape[1]
    taps = filter_taps[...].astype(f32)
    conv = branch_x.astype(f32) * taps[TAPS - 1 : TAPS]
    for j in range(TAPS - 1):
        conv = conv + recent[:, j * rnn : (j + 1) * rnn].astype(f32) * taps[j : j + 1]
    conv_out = conv.astype(bf16)
    width = recurrence_map.shape[1]
    blocks = rnn // width
    rec = jnp.concatenate(
        [
            jnp.dot(conv_out[:, i * width : (i + 1) * width], recurrence_map[i], preferred_element_type=f32)
            for i in range(blocks)
        ],
        axis=1,
    )
    ing = jnp.concatenate(
        [
            jnp.dot(conv_out[:, i * width : (i + 1) * width], input_map[i], preferred_element_type=f32)
            for i in range(blocks)
        ],
        axis=1,
    )
    rec_gate = jax.nn.sigmoid(rec)
    in_gate = jax.nn.sigmoid(ing)
    neg = -decay_param[...]
    soft = jnp.maximum(neg, 0.0) + jnp.log1p(jnp.exp(-jnp.abs(neg)))
    log_decay = -rate_scale * rec_gate * soft
    decay = jnp.exp(log_decay)
    lost = -jnp.tanh(log_decay) * (decay * decay + 1.0)
    new_hidden = decay * hidden_state[...] + jnp.sqrt(lost) * (in_gate * conv_out.astype(f32))
    new_hidden_out[...] = new_hidden
    branch_g = streamed(normed, w_branch, branch_loads).astype(bf16).astype(f32)
    mixed = (new_hidden * jax.nn.gelu(branch_g, approximate=True)).astype(bf16)
    after = resid + streamed(mixed, w_out, out_loads)
    after_ref[...] = after
    expert_in = rms_scale(after, gain_experts[...]).astype(bf16)

    seq = expert_in.shape[0]
    slots = EXPERTS * CAP
    col = lax.broadcasted_iota(jnp.int32, (seq, slots), 1)
    first = routes[:, 0:1]
    second = routes[:, 1:2]
    pick0 = (col // CAP) == first
    pick1 = (col // CAP) == second
    member = (pick0 | pick1).astype(f32)
    tri = (
        lax.broadcasted_iota(jnp.int32, (seq, seq), 0) >= lax.broadcasted_iota(jnp.int32, (seq, seq), 1)
    ).astype(f32)
    rank = jnp.dot(tri.astype(bf16), member.astype(bf16), preferred_element_type=f32)
    table = jnp.where(rank == (col % CAP + 1).astype(f32), member, 0.0)

    dense = lax.dot_general(
        table.astype(bf16), expert_in, (((0,), (0,)), ((), ())), preferred_element_type=f32
    )
    packed[...] = dense.reshape(packed.shape).astype(bf16)

    pl.semaphore_wait(barrier, len(peers))

    sends = []
    for k in ORDER:
        f = flip(e, k)
        copy = remote(packed.at[f], x_blocks.at[0, 0, e], d1_s.at[k], d1_r.at[k], f * group + q)
        copy.start()
        sends.append(copy)
    x_blocks[0, 0, e] = packed[e]

    logits = jnp.dot(expert_in, router_weight[...], preferred_element_type=f32)
    ids = lax.broadcasted_iota(jnp.int32, logits.shape, 1)
    l0 = jnp.sum(jnp.where(ids == first, logits, 0.0), axis=1, keepdims=True)
    l1 = jnp.sum(jnp.where(ids == second, logits, 0.0), axis=1, keepdims=True)
    share0 = jax.nn.sigmoid(l0 - l1)
    share1 = jax.nn.sigmoid(l1 - l0)
    scaled = table * (jnp.where(pick0, share0, 0.0) + jnp.where(pick1, share1, 0.0))
    high = scaled.astype(bf16)
    low = (scaled - high.astype(f32)).astype(bf16)
    combine = jnp.concatenate([high, low], axis=0)

    def spread(k):
        f = flip(e, k)
        for d in range(1, chips):
            copy = remote(
                x_blocks.at[0, 0, f],
                x_blocks.at[0, chips - d, f],
                d2_s.at[d - 1, k],
                d2_r.at[chips - d - 1, k],
                peer_chip(d),
            )
            copy.start()
            sends.append(copy)
        copy = remote(x_blocks.at[0, 0, f], x_blocks.at[1, 0, f], d3_s.at[0, k], d3_r.at[0, k], partner)
        copy.start()
        sends.append(copy)

    def arrived(buf, ssem, rsem):
        remote(buf, buf, ssem, rsem, partner).wait_recv()

    spread(0)
    for k in ORDER:
        arrived(x_blocks.at[0, 0, flip(e, k)], d1_s.at[k], d1_r.at[k])
        spread(k)

    block_rows = EXPERTS * CAP
    model = x_rows.shape[1]

    def flatten(c, d):
        at = (c * chips + d) * block_rows
        x_rows[at : at + block_rows, :] = (
            x_blocks[c, d].astype(f32).reshape(block_rows, model).astype(bf16)
        )

    for k in (0,) + ORDER:
        for d in range(1, chips):
            f = flip(e, k)
            arrived(x_blocks.at[0, d, f], d2_s.at[d - 1, k], d2_r.at[d - 1, k])
            copy = remote(x_blocks.at[0, d, f], x_blocks.at[1, d, f], d3_s.at[d, k], d3_r.at[d, k], partner)
            copy.start()
            sends.append(copy)
    for d in range(chips):
        flatten(0, d)
    for d in range(chips):
        for k in (0,) + ORDER:
            arrived(x_blocks.at[1, d, flip(e, k)], d3_s.at[d, k], d3_r.at[d, k])
        flatten(1, d)

    for copy in expert_loads:
        copy.wait()
    hidden = w_gate.shape[1]
    step = min(256, hidden)

    def hidden_chunk(j, carry):
        cut = pl.ds(pl.multiple_of(j * step, step), step)
        rows = x_rows[...]
        gate = jnp.dot(rows, w_gate[:, cut], preferred_element_type=f32)
        upper = jnp.dot(rows, w_up[:, cut], preferred_element_type=f32)
        inner[:, cut] = (gate * jax.nn.sigmoid(gate) * upper).astype(bf16)
        return carry

    lax.fori_loop(0, hidden // step, hidden_chunk, 0)

    half = chips * block_rows
    wide = model // n_col

    def down(c):
        out = jnp.dot(inner[...], w_down[:, c * wide : (c + 1) * wide], preferred_element_type=f32)
        a_send[c] = out[half:, :].astype(bf16)
        keep[c] = out[:half, :]
        copy = remote(a_send.at[c], a_recv.at[c], a_s.at[c], a_r.at[c], partner)
        copy.start()
        sends.append(copy)

    def across(c):
        arrived(a_recv.at[c], a_s.at[c], a_r.at[c])
        both = keep[c] + a_recv[c].astype(f32)
        for d in range(1, chips):
            b_send[d - 1, c] = both[d * block_rows : (d + 1) * block_rows, :].astype(bf16)
            copy = remote(
                b_send.at[d - 1, c],
                b_recv.at[chips - d - 1, c],
                b_s.at[d - 1, c],
                b_r.at[chips - d - 1, c],
                peer_chip(d),
            )
            copy.start()
            sends.append(copy)
        keep_own[c] = both[:block_rows, :]

    def home(c):
        total = keep_own[c]
        for d in range(1, chips):
            arrived(b_recv.at[d - 1, c], b_s.at[d - 1, c], b_r.at[d - 1, c])
            total = total + b_recv[d - 1, c].astype(f32)
        c_send[c] = total.reshape(EXPERTS, CAP, wide).astype(bf16)
        for k in ORDER:
            f = flip(e, k)
            copy = remote(c_send.at[c, f], c_recv.at[c, e], c_s.at[k, c], c_r.at[k, c], f * group + q)
            copy.start()
            sends.append(copy)
        c_recv[c, e] = c_send[c, e]

    def finish(c):
        for k in ORDER:
            arrived(c_recv.at[c, flip(e, k)], c_s.at[k, c], c_r.at[k, c])
        results = c_recv[c].astype(f32).reshape(slots, wide).astype(bf16)
        both = jnp.dot(combine, results, preferred_element_type=f32)
        cut = slice(c * wide, (c + 1) * wide)
        layer_out[:, cut] = (after_ref[:, cut] + (both[:seq] + both[seq:])).astype(bf16)

    for c in range(n_col):
        down(c)
        if c:
            across(c - 1)
    across(n_col - 1)
    for c in range(n_col):
        home(c)
    for c in range(n_col):
        finish(c)
    for copy in sends:
        copy.wait_send()


def solution(mesh):
    n = mesh.shape["ep"]

    def local(
        tokens,
        hidden_state,
        recent_inputs,
        routes,
        gain_mix,
        input_weight,
        branch_weight,
        filter_taps,
        recurrence_map,
        input_map,
        decay_param,
        output_weight,
        gain_experts,
        router_weight,
        expert_gate,
        expert_up,
        expert_down,
    ):
        seq, model = tokens.shape
        rnn = hidden_state.shape[1]
        hidden = expert_gate.shape[1]
        group = n // EXPERTS
        chips = group // 2
        rows = n * CAP
        block = EXPERTS * CAP
        n_col = 4
        wide = model // n_col
        dma = pltpu.SemaphoreType.DMA
        vmem = pl.BlockSpec(memory_space=pltpu.VMEM)
        hbm = pl.BlockSpec(memory_space=pl.ANY)
        far = max(chips - 1, 1)
        layer_out, new_hidden, branch_x = pl.pallas_call(
            functools.partial(kernel, n, n_col),
            out_shape=(
                jax.ShapeDtypeStruct((seq, model), bf16),
                jax.ShapeDtypeStruct((seq, rnn), f32),
                jax.ShapeDtypeStruct((seq, rnn), bf16),
            ),
            in_specs=[vmem] * 11 + [hbm] * 6,
            out_specs=(vmem, vmem, vmem),
            scratch_shapes=[
                pltpu.VMEM(input_weight.shape, bf16),
                pltpu.VMEM(branch_weight.shape, bf16),
                pltpu.VMEM(output_weight.shape, bf16),
                pltpu.VMEM(expert_gate.shape, bf16),
                pltpu.VMEM(expert_up.shape, bf16),
                pltpu.VMEM(expert_down.shape, bf16),
                pltpu.VMEM((seq, model), f32),
                pltpu.VMEM((EXPERTS, CAP, model), bf16),
                pltpu.VMEM((2, chips, EXPERTS, CAP, model), bf16),
                pltpu.VMEM((rows, model), bf16),
                pltpu.VMEM((rows, hidden), bf16),
                pltpu.VMEM((n_col, rows // 2, wide), bf16),
                pltpu.VMEM((n_col, rows // 2, wide), bf16),
                pltpu.VMEM((n_col, rows // 2, wide), f32),
                pltpu.VMEM((far, n_col, block, wide), bf16),
                pltpu.VMEM((far, n_col, block, wide), bf16),
                pltpu.VMEM((n_col, block, wide), f32),
                pltpu.VMEM((n_col, EXPERTS, CAP, wide), bf16),
                pltpu.VMEM((n_col, EXPERTS, CAP, wide), bf16),
                dma((16,)),
                dma((EXPERTS,)),
                dma((EXPERTS,)),
                dma((far, EXPERTS)),
                dma((far, EXPERTS)),
                dma((chips, EXPERTS)),
                dma((chips, EXPERTS)),
                dma((n_col,)),
                dma((n_col,)),
                dma((far, n_col)),
                dma((far, n_col)),
                dma((EXPERTS, n_col)),
                dma((EXPERTS, n_col)),
            ],
            compiler_params=pltpu.CompilerParams(
                collective_id=0, has_side_effects=True, vmem_limit_bytes=60 * 1024 * 1024
            ),
        )(
            tokens,
            hidden_state,
            recent_inputs.reshape(seq, -1),
            routes,
            gain_mix[None],
            filter_taps,
            recurrence_map,
            input_map,
            decay_param[None],
            gain_experts[None],
            router_weight,
            input_weight,
            branch_weight,
            output_weight,
            expert_gate,
            expert_up,
            expert_down,
        )
        new_inputs = jnp.concatenate([recent_inputs[:, 1:, :], branch_x[:, None, :]], axis=1)
        return (layer_out, new_hidden, new_inputs)

    placed = (
        P("ep", None),
        P("ep", None),
        P("ep", None, None),
        P("ep", None),
    ) + (P(),) * 10 + (P(None, "ep"), P(None, "ep"), P("ep", None))
    return jax.shard_map(
        local,
        mesh=mesh,
        in_specs=placed,
        out_specs=(P("ep", None), P("ep", None), P("ep", None, None)),
        check_vma=False,
    )
```

```python
import functools

import jax
import jax.numpy as jnp
from jax import lax
from jax.experimental import pallas as pl
from jax.experimental.pallas import tpu as pltpu
from jax.sharding import PartitionSpec as P

EXPERTS = 8
CAP = 8
TAPS = 4
BITS = 3
ORDER = (1, 4, 2, 6, 3, 5, 7)

epsilon = 1e-06
rate_scale = 8.0

f32 = jnp.float32
bf16 = jnp.bfloat16


def rms_scale(values, gain):
    mean_square = jnp.mean(values * values, axis=-1, keepdims=True)
    return values * lax.rsqrt(mean_square + epsilon) * gain.astype(f32)


def as_row(blocks):
    values = blocks[...].astype(f32)
    return jnp.concatenate([values[i : i + 1] for i in range(values.shape[0])], axis=1)


def write_out(layer, hidden, branch_x, recent, layer_out, hidden_out, inputs_out):
    layer_out[...] = layer[...]
    hidden_out[...] = hidden[...]
    for j in range(TAPS - 2):
        inputs_out[j] = recent[j + 1]
    inputs_out[TAPS - 2] = branch_x[...]


def flip(e, k):
    out = 0
    for i in range(BITS):
        bit = (e // (1 << i)) % 2
        if (k >> i) & 1:
            bit = 1 - bit
        out = out + bit * (1 << i)
    return out


def kernel(
    n,
    n_col,
    tokens,
    hidden_state,
    recent,
    routes,
    gain_mix,
    filter_taps,
    recurrence_map,
    input_map,
    decay_param,
    gain_experts,
    router_weight,
    w_in_hbm,
    w_branch_hbm,
    w_out_hbm,
    w_gate_hbm,
    w_up_hbm,
    w_down_hbm,
    layer_out,
    new_hidden_out,
    branch_out,
    w_in,
    w_branch,
    w_out,
    w_gate,
    w_up,
    w_down,
    after_ref,
    packed,
    x_blocks,
    x_rows,
    inner,
    a_send,
    a_recv,
    keep,
    b_send,
    b_recv,
    keep_own,
    c_send,
    c_recv,
    w_sem,
    d1_s,
    d1_r,
    d2_s,
    d2_r,
    d3_s,
    d3_r,
    a_s,
    a_r,
    b_s,
    b_r,
    c_s,
    c_r,
):
    me = lax.axis_index("ep")
    group = n // EXPERTS
    chips = group // 2
    e = me // group
    q = me % group
    core = me % 2
    chip = q // 2
    partner = me + 1 - 2 * core

    def peer_chip(d):
        return e * group + ((chip + d) % chips) * 2 + core

    def remote(src, dst, ssem, rsem, dev):
        return pltpu.make_async_remote_copy(
            src_ref=src,
            dst_ref=dst,
            send_sem=ssem,
            recv_sem=rsem,
            device_id=(dev,),
            device_id_type=pl.DeviceIdType.MESH,
        )

    barrier = pltpu.get_barrier_semaphore()
    peers = [flip(e, k) * group + q for k in range(1, EXPERTS)]
    peers += [partner] + [peer_chip(d) for d in range(1, chips)]
    for dev in peers:
        pl.semaphore_signal(
            barrier, inc=1, device_id=(dev,), device_id_type=pl.DeviceIdType.MESH
        )

    parts = 4
    loads = []

    def load(src, dst, pieces):
        rows = src.shape[0] // pieces
        made = []
        for i in range(pieces):
            cut = pl.ds(i * rows, rows)
            made.append(pltpu.make_async_copy(src.at[cut], dst.at[cut], w_sem.at[len(loads)]))
            loads.append(made[-1])
        return made

    in_loads = load(w_in_hbm, w_in, parts)
    branch_loads = load(w_branch_hbm, w_branch, parts)
    out_loads = load(w_out_hbm, w_out, parts)
    expert_loads = load(w_gate_hbm, w_gate, 1) + load(w_up_hbm, w_up, 1) + load(w_down_hbm, w_down, 1)
    for copy in in_loads + branch_loads + out_loads:
        copy.start()

    def streamed(lhs, weight, copies):
        rows = weight.shape[0] // len(copies)
        total = None
        for i, copy in enumerate(copies):
            copy.wait()
            part = jnp.dot(
                lhs[:, i * rows : (i + 1) * rows],
                weight[i * rows : (i + 1) * rows, :],
                preferred_element_type=f32,
            )
            total = part if total is None else total + part
        return total

    resid = tokens[...].astype(f32)
    normed = rms_scale(resid, as_row(gain_mix)).astype(bf16)
    branch_x = streamed(normed, w_in, in_loads).astype(bf16)
    branch_out[...] = branch_x
    rnn = branch_x.shape[1]
    taps = filter_taps[...].astype(f32)
    conv = branch_x.astype(f32) * taps[TAPS - 1 : TAPS]
    for j in range(TAPS - 1):
        conv = conv + recent[j].astype(f32) * taps[j : j + 1]
    conv_out = conv.astype(bf16)
    width = recurrence_map.shape[1]
    blocks = rnn // width
    rec = jnp.concatenate(
        [
            jnp.dot(conv_out[:, i * width : (i + 1) * width], recurrence_map[i], preferred_element_type=f32)
            for i in range(blocks)
        ],
        axis=1,
    )
    ing = jnp.concatenate(
        [
            jnp.dot(conv_out[:, i * width : (i + 1) * width], input_map[i], preferred_element_type=f32)
            for i in range(blocks)
        ],
        axis=1,
    )
    rec_gate = jax.nn.sigmoid(rec)
    in_gate = jax.nn.sigmoid(ing)
    neg = -decay_param[...]
    soft = jnp.maximum(neg, 0.0) + jnp.log1p(jnp.exp(-jnp.abs(neg)))
    log_decay = -rate_scale * rec_gate * soft
    decay = jnp.exp(log_decay)
    lost = -jnp.tanh(log_decay) * (decay * decay + 1.0)
    new_hidden = decay * hidden_state[...] + jnp.sqrt(lost) * (in_gate * conv_out.astype(f32))
    new_hidden_out[...] = new_hidden
    branch_g = streamed(normed, w_branch, branch_loads).astype(bf16).astype(f32)
    for copy in expert_loads:
        copy.start()
    mixed = (new_hidden * jax.nn.gelu(branch_g, approximate=True)).astype(bf16)
    after = resid + streamed(mixed, w_out, out_loads)
    after_ref[...] = after
    expert_in = rms_scale(after, as_row(gain_experts)).astype(bf16)

    seq = expert_in.shape[0]
    slots = EXPERTS * CAP
    row = lax.broadcasted_iota(jnp.int32, (slots, seq), 0)
    first = routes[0:1, :]
    second = routes[1:2, :]
    pick0 = (row // CAP) == first
    pick1 = (row // CAP) == second
    member = (pick0 | pick1).astype(f32)
    tri = (
        lax.broadcasted_iota(jnp.int32, (seq, seq), 0) <= lax.broadcasted_iota(jnp.int32, (seq, seq), 1)
    ).astype(f32)
    rank = jnp.dot(member.astype(bf16), tri.astype(bf16), preferred_element_type=f32)
    table = jnp.where(rank == (row % CAP + 1).astype(f32), member, 0.0)

    dense = jnp.dot(table.astype(bf16), expert_in, preferred_element_type=f32)
    packed[...] = dense.reshape(packed.shape).astype(bf16)

    pl.semaphore_wait(barrier, len(peers))

    sends = []
    for k in ORDER:
        f = flip(e, k)
        copy = remote(packed.at[f], x_blocks.at[0, 0, e], d1_s.at[k], d1_r.at[k], f * group + q)
        copy.start()
        sends.append(copy)
    x_blocks[0, 0, e] = packed[e]

    logits = lax.dot_general(
        router_weight[...], expert_in, (((1,), (1,)), ((), ())), preferred_element_type=f32
    )
    ids = lax.broadcasted_iota(jnp.int32, logits.shape, 0)
    l0 = jnp.sum(jnp.where(ids == first, logits, 0.0), axis=0, keepdims=True)
    l1 = jnp.sum(jnp.where(ids == second, logits, 0.0), axis=0, keepdims=True)
    share0 = jax.nn.sigmoid(l0 - l1)
    share1 = jax.nn.sigmoid(l1 - l0)
    scaled = table * (jnp.where(pick0, share0, 0.0) + jnp.where(pick1, share1, 0.0))
    scaled = scaled.T
    high = scaled.astype(bf16)
    low = (scaled - high.astype(f32)).astype(bf16)
    combine = jnp.concatenate([high, low], axis=0)

    def spread(k):
        f = flip(e, k)
        for d in range(1, chips):
            copy = remote(
                x_blocks.at[0, 0, f],
                x_blocks.at[0, chips - d, f],
                d2_s.at[d - 1, k],
                d2_r.at[chips - d - 1, k],
                peer_chip(d),
            )
            copy.start()
            sends.append(copy)
        copy = remote(x_blocks.at[0, 0, f], x_blocks.at[1, 0, f], d3_s.at[0, k], d3_r.at[0, k], partner)
        copy.start()
        sends.append(copy)

    def arrived(buf, ssem, rsem):
        remote(buf, buf, ssem, rsem, partner).wait_recv()

    spread(0)
    for k in ORDER:
        arrived(x_blocks.at[0, 0, flip(e, k)], d1_s.at[k], d1_r.at[k])
        spread(k)

    block_rows = EXPERTS * CAP
    model = x_rows.shape[1]

    def flatten(c, d):
        at = (c * chips + d) * block_rows
        x_rows[at : at + block_rows, :] = (
            x_blocks[c, d].astype(f32).reshape(block_rows, model).astype(bf16)
        )

    for k in (0,) + ORDER:
        for d in range(1, chips):
            f = flip(e, k)
            arrived(x_blocks.at[0, d, f], d2_s.at[d - 1, k], d2_r.at[d - 1, k])
            copy = remote(x_blocks.at[0, d, f], x_blocks.at[1, d, f], d3_s.at[d, k], d3_r.at[d, k], partner)
            copy.start()
            sends.append(copy)
    for d in range(chips):
        flatten(0, d)
    for d in range(chips):
        for k in (0,) + ORDER:
            arrived(x_blocks.at[1, d, flip(e, k)], d3_s.at[d, k], d3_r.at[d, k])
        flatten(1, d)

    for copy in expert_loads:
        copy.wait()
    hidden = w_gate.shape[1]
    step = min(256, hidden)

    def hidden_chunk(j, carry):
        cut = pl.ds(pl.multiple_of(j * step, step), step)
        rows = x_rows[...]
        gate = jnp.dot(rows, w_gate[:, cut], preferred_element_type=f32)
        upper = jnp.dot(rows, w_up[:, cut], preferred_element_type=f32)
        inner[:, cut] = (gate * jax.nn.sigmoid(gate) * upper).astype(bf16)
        return carry

    lax.fori_loop(0, hidden // step, hidden_chunk, 0)

    half = chips * block_rows
    wide = model // n_col

    def down(c):
        out = jnp.dot(inner[...], w_down[:, c * wide : (c + 1) * wide], preferred_element_type=f32)
        a_send[c] = out[half:, :].astype(bf16)
        keep[c] = out[:half, :]
        copy = remote(a_send.at[c], a_recv.at[c], a_s.at[c], a_r.at[c], partner)
        copy.start()
        sends.append(copy)

    def across(c):
        arrived(a_recv.at[c], a_s.at[c], a_r.at[c])
        both = keep[c] + a_recv[c].astype(f32)
        for d in range(1, chips):
            b_send[d - 1, c] = both[d * block_rows : (d + 1) * block_rows, :].astype(bf16)
            copy = remote(
                b_send.at[d - 1, c],
                b_recv.at[chips - d - 1, c],
                b_s.at[d - 1, c],
                b_r.at[chips - d - 1, c],
                peer_chip(d),
            )
            copy.start()
            sends.append(copy)
        keep_own[c] = both[:block_rows, :]

    def home(c):
        total = keep_own[c]
        for d in range(1, chips):
            arrived(b_recv.at[d - 1, c], b_s.at[d - 1, c], b_r.at[d - 1, c])
            total = total + b_recv[d - 1, c].astype(f32)
        c_send[c] = total.reshape(EXPERTS, CAP, wide).astype(bf16)
        for k in ORDER:
            f = flip(e, k)
            copy = remote(c_send.at[c, f], c_recv.at[c, e], c_s.at[k, c], c_r.at[k, c], f * group + q)
            copy.start()
            sends.append(copy)
        c_recv[c, e] = c_send[c, e]

    def finish(c):
        for k in ORDER:
            arrived(c_recv.at[c, flip(e, k)], c_s.at[k, c], c_r.at[k, c])
        results = c_recv[c].astype(f32).reshape(slots, wide).astype(bf16)
        both = jnp.dot(combine, results, preferred_element_type=f32)
        cut = slice(c * wide, (c + 1) * wide)
        layer_out[:, cut] = (after_ref[:, cut] + (both[:seq] + both[seq:])).astype(bf16)

    for c in range(n_col):
        down(c)
        if c:
            across(c - 1)
    across(n_col - 1)
    for c in range(n_col):
        home(c)
    for c in range(n_col):
        finish(c)
    for copy in sends:
        copy.wait_send()


def solution(mesh):
    n = mesh.shape["ep"]

    def local(
        tokens,
        hidden_state,
        recent_inputs,
        routes,
        gain_mix,
        input_weight,
        branch_weight,
        filter_taps,
        recurrence_map,
        input_map,
        decay_param,
        output_weight,
        gain_experts,
        router_weight,
        expert_gate,
        expert_up,
        expert_down,
    ):
        seq, model = tokens.shape
        rnn = hidden_state.shape[1]
        hidden = expert_gate.shape[1]
        group = n // EXPERTS
        chips = group // 2
        rows = n * CAP
        block = EXPERTS * CAP
        n_col = 8
        wide = model // n_col
        dma = pltpu.SemaphoreType.DMA
        vmem = pl.BlockSpec(memory_space=pltpu.VMEM)
        hbm = pl.BlockSpec(memory_space=pltpu.HBM)
        far = max(chips - 1, 1)
        recent = jnp.transpose(recent_inputs, (1, 0, 2))
        layer_out, new_hidden, branch_x = pl.pallas_call(
            functools.partial(kernel, n, n_col),
            out_shape=(
                pltpu.VMEM((seq, model), bf16),
                pltpu.VMEM((seq, rnn), f32),
                pltpu.VMEM((seq, rnn), bf16),
            ),
            in_specs=[vmem] * 11 + [hbm] * 6,
            out_specs=(vmem, vmem, vmem),
            scratch_shapes=[
                pltpu.VMEM(input_weight.shape, bf16),
                pltpu.VMEM(branch_weight.shape, bf16),
                pltpu.VMEM(output_weight.shape, bf16),
                pltpu.VMEM(expert_gate.shape, bf16),
                pltpu.VMEM(expert_up.shape, bf16),
                pltpu.VMEM(expert_down.shape, bf16),
                pltpu.VMEM((seq, model), f32),
                pltpu.VMEM((EXPERTS, CAP, model), bf16),
                pltpu.VMEM((2, chips, EXPERTS, CAP, model), bf16),
                pltpu.VMEM((rows, model), bf16),
                pltpu.VMEM((rows, hidden), bf16),
                pltpu.VMEM((n_col, rows // 2, wide), bf16),
                pltpu.VMEM((n_col, rows // 2, wide), bf16),
                pltpu.VMEM((n_col, rows // 2, wide), f32),
                pltpu.VMEM((far, n_col, block, wide), bf16),
                pltpu.VMEM((far, n_col, block, wide), bf16),
                pltpu.VMEM((n_col, block, wide), f32),
                pltpu.VMEM((n_col, EXPERTS, CAP, wide), bf16),
                pltpu.VMEM((n_col, EXPERTS, CAP, wide), bf16),
                dma((16,)),
                dma((EXPERTS,)),
                dma((EXPERTS,)),
                dma((far, EXPERTS)),
                dma((far, EXPERTS)),
                dma((chips, EXPERTS)),
                dma((chips, EXPERTS)),
                dma((n_col,)),
                dma((n_col,)),
                dma((far, n_col)),
                dma((far, n_col)),
                dma((EXPERTS, n_col)),
                dma((EXPERTS, n_col)),
            ],
            compiler_params=pltpu.CompilerParams(
                collective_id=0, has_side_effects=True, vmem_limit_bytes=61 * 1024 * 1024
            ),
        )(
            tokens,
            hidden_state,
            recent,
            routes.T,
            gain_mix.reshape(-1, 128),
            filter_taps,
            recurrence_map,
            input_map,
            decay_param[None],
            gain_experts.reshape(-1, 128),
            router_weight.T,
            input_weight,
            branch_weight,
            output_weight,
            expert_gate,
            expert_up,
            expert_down,
        )
        layer_out, new_hidden, new_inputs = pl.pallas_call(
            write_out,
            out_shape=(
                jax.ShapeDtypeStruct((seq, model), bf16),
                jax.ShapeDtypeStruct((seq, rnn), f32),
                jax.ShapeDtypeStruct(recent.shape, bf16),
            ),
            in_specs=[vmem] * 4,
            out_specs=(vmem, vmem, vmem),
            compiler_params=pltpu.CompilerParams(vmem_limit_bytes=4 * 1024 * 1024),
        )(layer_out, new_hidden, branch_x, recent)
        return (layer_out, new_hidden, jnp.transpose(new_inputs, (1, 0, 2)))

    placed = (
        P("ep", None),
        P("ep", None),
        P("ep", None, None),
        P("ep", None),
    ) + (P(),) * 10 + (P(None, "ep"), P(None, "ep"), P("ep", None))
    return jax.shard_map(
        local,
        mesh=mesh,
        in_specs=placed,
        out_specs=(P("ep", None), P("ep", None), P("ep", None, None)),
        check_vma=False,
    )
```

```python
import functools

import jax
import jax.numpy as jnp
from jax import lax
from jax.experimental import pallas as pl
from jax.experimental.pallas import tpu as pltpu
from jax.sharding import PartitionSpec as P

EXPERTS = 8
CAP = 8
TAPS = 4
BITS = 3
ORDER = (1, 4, 2, 6, 3, 5, 7)

epsilon = 1e-06
rate_scale = 8.0

f32 = jnp.float32
bf16 = jnp.bfloat16


def rms_scale(values, gain):
    mean_square = jnp.mean(values * values, axis=-1, keepdims=True)
    return values * lax.rsqrt(mean_square + epsilon) * gain.astype(f32)


def as_row(blocks):
    values = blocks[...].astype(f32)
    return jnp.concatenate([values[i : i + 1] for i in range(values.shape[0])], axis=1)


def write_out(layer, hidden, branch_x, recent, layer_out, hidden_out, inputs_out):
    layer_out[...] = layer[...]
    hidden_out[...] = hidden[...]
    for j in range(TAPS - 2):
        inputs_out[j] = recent[j + 1]
    inputs_out[TAPS - 2] = branch_x[...]


def flip(e, k):
    out = 0
    for i in range(BITS):
        bit = (e // (1 << i)) % 2
        if (k >> i) & 1:
            bit = 1 - bit
        out = out + bit * (1 << i)
    return out


def kernel(
    n,
    n_col,
    tokens_hbm,
    hidden_state_hbm,
    recent_hbm,
    routes_hbm,
    gain_mix_hbm,
    filter_taps_hbm,
    recurrence_map_hbm,
    input_map_hbm,
    decay_param_hbm,
    gain_experts_hbm,
    router_weight_hbm,
    w_in_hbm,
    w_branch_hbm,
    w_out_hbm,
    w_gate_hbm,
    w_up_hbm,
    w_down_hbm,
    layer_out,
    new_hidden_out,
    branch_out,
    tokens,
    hidden_state,
    recent,
    routes,
    gain_mix,
    filter_taps,
    recurrence_map,
    input_map,
    decay_param,
    gain_experts,
    router_weight,
    w_in,
    w_branch,
    w_out,
    w_gate,
    w_up,
    w_down,
    after_ref,
    packed,
    x_blocks,
    x_rows,
    inner,
    a_send,
    a_recv,
    keep,
    b_send,
    b_recv,
    keep_own,
    c_send,
    c_recv,
    w_sem,
    d1_s,
    d1_r,
    d2_s,
    d2_r,
    d3_s,
    d3_r,
    a_s,
    a_r,
    b_s,
    b_r,
    c_s,
    c_r,
    small_sem,
):
    me = lax.axis_index("ep")
    group = n // EXPERTS
    chips = group // 2
    e = me // group
    q = me % group
    core = me % 2
    chip = q // 2
    partner = me + 1 - 2 * core

    def peer_chip(d):
        return e * group + ((chip + d) % chips) * 2 + core

    def remote(src, dst, ssem, rsem, dev):
        return pltpu.make_async_remote_copy(
            src_ref=src,
            dst_ref=dst,
            send_sem=ssem,
            recv_sem=rsem,
            device_id=(dev,),
            device_id_type=pl.DeviceIdType.MESH,
        )

    barrier = pltpu.get_barrier_semaphore()
    peers = [flip(e, k) * group + q for k in range(1, EXPERTS)]
    peers += [partner] + [peer_chip(d) for d in range(1, chips)]
    for dev in peers:
        pl.semaphore_signal(
            barrier, inc=1, device_id=(dev,), device_id_type=pl.DeviceIdType.MESH
        )

    small = [
        (tokens_hbm, tokens),
        (gain_mix_hbm, gain_mix),
        (hidden_state_hbm, hidden_state),
        (recent_hbm, recent),
        (routes_hbm, routes),
        (filter_taps_hbm, filter_taps),
        (recurrence_map_hbm, recurrence_map),
        (input_map_hbm, input_map),
        (decay_param_hbm, decay_param),
        (gain_experts_hbm, gain_experts),
        (router_weight_hbm, router_weight),
    ]
    small = [pltpu.make_async_copy(src, dst, small_sem.at[i]) for i, (src, dst) in enumerate(small)]
    for copy in small:
        copy.start()
    parts = 4
    loads = []

    def load(src, dst, pieces):
        rows = src.shape[0] // pieces
        made = []
        for i in range(pieces):
            cut = pl.ds(i * rows, rows)
            made.append(pltpu.make_async_copy(src.at[cut], dst.at[cut], w_sem.at[len(loads)]))
            loads.append(made[-1])
        return made

    in_loads = load(w_in_hbm, w_in, parts)
    branch_loads = load(w_branch_hbm, w_branch, parts)
    out_loads = load(w_out_hbm, w_out, parts)
    expert_loads = load(w_gate_hbm, w_gate, 1) + load(w_up_hbm, w_up, 1) + load(w_down_hbm, w_down, 1)
    for copy in in_loads + branch_loads + out_loads:
        copy.start()

    def streamed(lhs, weight, copies):
        rows = weight.shape[0] // len(copies)
        total = None
        for i, copy in enumerate(copies):
            copy.wait()
            part = jnp.dot(
                lhs[:, i * rows : (i + 1) * rows],
                weight[i * rows : (i + 1) * rows, :],
                preferred_element_type=f32,
            )
            total = part if total is None else total + part
        return total

    for copy in small[:2]:
        copy.wait()
    resid = tokens[...].astype(f32)
    normed = rms_scale(resid, as_row(gain_mix)).astype(bf16)
    branch_x = streamed(normed, w_in, in_loads).astype(bf16)
    branch_out[...] = branch_x
    for copy in small[2:]:
        copy.wait()
    rnn = branch_x.shape[1]
    taps = filter_taps[...].astype(f32)
    conv = branch_x.astype(f32) * taps[TAPS - 1 : TAPS]
    for j in range(TAPS - 1):
        conv = conv + recent[j].astype(f32) * taps[j : j + 1]
    conv_out = conv.astype(bf16)
    width = recurrence_map.shape[1]
    blocks = rnn // width
    rec = jnp.concatenate(
        [
            jnp.dot(conv_out[:, i * width : (i + 1) * width], recurrence_map[i], preferred_element_type=f32)
            for i in range(blocks)
        ],
        axis=1,
    )
    ing = jnp.concatenate(
        [
            jnp.dot(conv_out[:, i * width : (i + 1) * width], input_map[i], preferred_element_type=f32)
            for i in range(blocks)
        ],
        axis=1,
    )
    rec_gate = jax.nn.sigmoid(rec)
    in_gate = jax.nn.sigmoid(ing)
    neg = -decay_param[...]
    soft = jnp.maximum(neg, 0.0) + jnp.log1p(jnp.exp(-jnp.abs(neg)))
    log_decay = -rate_scale * rec_gate * soft
    decay = jnp.exp(log_decay)
    lost = -jnp.tanh(log_decay) * (decay * decay + 1.0)
    new_hidden = decay * hidden_state[...] + jnp.sqrt(lost) * (in_gate * conv_out.astype(f32))
    new_hidden_out[...] = new_hidden
    branch_g = streamed(normed, w_branch, branch_loads).astype(bf16).astype(f32)
    for copy in expert_loads:
        copy.start()
    mixed = (new_hidden * jax.nn.gelu(branch_g, approximate=True)).astype(bf16)
    after = resid + streamed(mixed, w_out, out_loads)
    after_ref[...] = after
    expert_in = rms_scale(after, as_row(gain_experts)).astype(bf16)

    seq = expert_in.shape[0]
    slots = EXPERTS * CAP
    row = lax.broadcasted_iota(jnp.int32, (slots, seq), 0)
    first = routes[0:1, :]
    second = routes[1:2, :]
    pick0 = (row // CAP) == first
    pick1 = (row // CAP) == second
    member = (pick0 | pick1).astype(f32)
    tri = (
        lax.broadcasted_iota(jnp.int32, (seq, seq), 0) <= lax.broadcasted_iota(jnp.int32, (seq, seq), 1)
    ).astype(f32)
    rank = jnp.dot(member.astype(bf16), tri.astype(bf16), preferred_element_type=f32)
    table = jnp.where(rank == (row % CAP + 1).astype(f32), member, 0.0)

    dense = jnp.dot(table.astype(bf16), expert_in, preferred_element_type=f32)
    packed[...] = dense.reshape(packed.shape).astype(bf16)

    pl.semaphore_wait(barrier, len(peers))

    sends = []
    for k in ORDER:
        f = flip(e, k)
        copy = remote(packed.at[f], x_blocks.at[0, 0, e], d1_s.at[k], d1_r.at[k], f * group + q)
        copy.start()
        sends.append(copy)
    x_blocks[0, 0, e] = packed[e]

    logits = lax.dot_general(
        router_weight[...], expert_in, (((1,), (1,)), ((), ())), preferred_element_type=f32
    )
    ids = lax.broadcasted_iota(jnp.int32, logits.shape, 0)
    l0 = jnp.sum(jnp.where(ids == first, logits, 0.0), axis=0, keepdims=True)
    l1 = jnp.sum(jnp.where(ids == second, logits, 0.0), axis=0, keepdims=True)
    share0 = jax.nn.sigmoid(l0 - l1)
    share1 = jax.nn.sigmoid(l1 - l0)
    scaled = table * (jnp.where(pick0, share0, 0.0) + jnp.where(pick1, share1, 0.0))
    scaled = scaled.T
    high = scaled.astype(bf16)
    low = (scaled - high.astype(f32)).astype(bf16)
    combine = jnp.concatenate([high, low], axis=0)

    def spread(k):
        f = flip(e, k)
        for d in range(1, chips):
            copy = remote(
                x_blocks.at[0, 0, f],
                x_blocks.at[0, chips - d, f],
                d2_s.at[d - 1, k],
                d2_r.at[chips - d - 1, k],
                peer_chip(d),
            )
            copy.start()
            sends.append(copy)
        copy = remote(x_blocks.at[0, 0, f], x_blocks.at[1, 0, f], d3_s.at[0, k], d3_r.at[0, k], partner)
        copy.start()
        sends.append(copy)

    def arrived(buf, ssem, rsem):
        remote(buf, buf, ssem, rsem, partner).wait_recv()

    spread(0)
    for k in ORDER:
        arrived(x_blocks.at[0, 0, flip(e, k)], d1_s.at[k], d1_r.at[k])
        spread(k)

    block_rows = EXPERTS * CAP
    model = x_rows.shape[1]

    def flatten(c, d):
        at = (c * chips + d) * block_rows
        x_rows[at : at + block_rows, :] = (
            x_blocks[c, d].astype(f32).reshape(block_rows, model).astype(bf16)
        )

    for k in (0,) + ORDER:
        for d in range(1, chips):
            f = flip(e, k)
            arrived(x_blocks.at[0, d, f], d2_s.at[d - 1, k], d2_r.at[d - 1, k])
            copy = remote(x_blocks.at[0, d, f], x_blocks.at[1, d, f], d3_s.at[d, k], d3_r.at[d, k], partner)
            copy.start()
            sends.append(copy)
    for d in range(chips):
        flatten(0, d)
    for d in range(chips):
        for k in (0,) + ORDER:
            arrived(x_blocks.at[1, d, flip(e, k)], d3_s.at[d, k], d3_r.at[d, k])
        flatten(1, d)

    for copy in expert_loads:
        copy.wait()
    hidden = w_gate.shape[1]
    step = min(256, hidden)

    def hidden_chunk(j, carry):
        cut = pl.ds(pl.multiple_of(j * step, step), step)
        rows = x_rows[...]
        gate = jnp.dot(rows, w_gate[:, cut], preferred_element_type=f32)
        upper = jnp.dot(rows, w_up[:, cut], preferred_element_type=f32)
        inner[:, cut] = (gate * jax.nn.sigmoid(gate) * upper).astype(bf16)
        return carry

    lax.fori_loop(0, hidden // step, hidden_chunk, 0)

    half = chips * block_rows
    wide = model // n_col

    def down(c):
        out = jnp.dot(inner[...], w_down[:, c * wide : (c + 1) * wide], preferred_element_type=f32)
        a_send[c] = out[half:, :].astype(bf16)
        keep[c] = out[:half, :]
        copy = remote(a_send.at[c], a_recv.at[c], a_s.at[c], a_r.at[c], partner)
        copy.start()
        sends.append(copy)

    def across(c):
        arrived(a_recv.at[c], a_s.at[c], a_r.at[c])
        both = keep[c] + a_recv[c].astype(f32)
        for d in range(1, chips):
            b_send[d - 1, c] = both[d * block_rows : (d + 1) * block_rows, :].astype(bf16)
            copy = remote(
                b_send.at[d - 1, c],
                b_recv.at[chips - d - 1, c],
                b_s.at[d - 1, c],
                b_r.at[chips - d - 1, c],
                peer_chip(d),
            )
            copy.start()
            sends.append(copy)
        keep_own[c] = both[:block_rows, :]

    def home(c):
        total = keep_own[c]
        for d in range(1, chips):
            arrived(b_recv.at[d - 1, c], b_s.at[d - 1, c], b_r.at[d - 1, c])
            total = total + b_recv[d - 1, c].astype(f32)
        c_send[c] = total.reshape(EXPERTS, CAP, wide).astype(bf16)
        for k in ORDER:
            f = flip(e, k)
            copy = remote(c_send.at[c, f], c_recv.at[c, e], c_s.at[k, c], c_r.at[k, c], f * group + q)
            copy.start()
            sends.append(copy)
        c_recv[c, e] = c_send[c, e]

    def finish(c):
        for k in ORDER:
            arrived(c_recv.at[c, flip(e, k)], c_s.at[k, c], c_r.at[k, c])
        results = c_recv[c].astype(f32).reshape(slots, wide).astype(bf16)
        both = jnp.dot(combine, results, preferred_element_type=f32)
        cut = slice(c * wide, (c + 1) * wide)
        layer_out[:, cut] = (after_ref[:, cut] + (both[:seq] + both[seq:])).astype(bf16)

    for c in range(n_col):
        down(c)
        if c:
            across(c - 1)
    across(n_col - 1)
    for c in range(n_col):
        home(c)
    for c in range(n_col):
        finish(c)
    for copy in sends:
        copy.wait_send()


def solution(mesh):
    n = mesh.shape["ep"]

    def local(
        tokens,
        hidden_state,
        recent_inputs,
        routes,
        gain_mix,
        input_weight,
        branch_weight,
        filter_taps,
        recurrence_map,
        input_map,
        decay_param,
        output_weight,
        gain_experts,
        router_weight,
        expert_gate,
        expert_up,
        expert_down,
    ):
        seq, model = tokens.shape
        rnn = hidden_state.shape[1]
        hidden = expert_gate.shape[1]
        group = n // EXPERTS
        chips = group // 2
        rows = n * CAP
        block = EXPERTS * CAP
        n_col = 4
        wide = model // n_col
        dma = pltpu.SemaphoreType.DMA
        vmem = pl.BlockSpec(memory_space=pltpu.VMEM)
        hbm = pl.BlockSpec(memory_space=pltpu.HBM)
        far = max(chips - 1, 1)
        recent = jnp.transpose(recent_inputs, (1, 0, 2))
        small = (
            tokens,
            hidden_state,
            recent,
            routes.T,
            gain_mix.reshape(-1, 128),
            filter_taps,
            recurrence_map,
            input_map,
            decay_param[None],
            gain_experts.reshape(-1, 128),
            router_weight.T,
        )
        layer_out, new_hidden, branch_x = pl.pallas_call(
            functools.partial(kernel, n, n_col),
            out_shape=(
                pltpu.VMEM((seq, model), bf16),
                pltpu.VMEM((seq, rnn), f32),
                pltpu.VMEM((seq, rnn), bf16),
            ),
            in_specs=[hbm] * 17,
            out_specs=(vmem, vmem, vmem),
            scratch_shapes=[pltpu.VMEM(x.shape, x.dtype) for x in small]
            + [
                pltpu.VMEM(input_weight.shape, bf16),
                pltpu.VMEM(branch_weight.shape, bf16),
                pltpu.VMEM(output_weight.shape, bf16),
                pltpu.VMEM(expert_gate.shape, bf16),
                pltpu.VMEM(expert_up.shape, bf16),
                pltpu.VMEM(expert_down.shape, bf16),
                pltpu.VMEM((seq, model), f32),
                pltpu.VMEM((EXPERTS, CAP, model), bf16),
                pltpu.VMEM((2, chips, EXPERTS, CAP, model), bf16),
                pltpu.VMEM((rows, model), bf16),
                pltpu.VMEM((rows, hidden), bf16),
                pltpu.VMEM((n_col, rows // 2, wide), bf16),
                pltpu.VMEM((n_col, rows // 2, wide), bf16),
                pltpu.VMEM((n_col, rows // 2, wide), f32),
                pltpu.VMEM((far, n_col, block, wide), bf16),
                pltpu.VMEM((far, n_col, block, wide), bf16),
                pltpu.VMEM((n_col, block, wide), f32),
                pltpu.VMEM((n_col, EXPERTS, CAP, wide), bf16),
                pltpu.VMEM((n_col, EXPERTS, CAP, wide), bf16),
                dma((16,)),
                dma((EXPERTS,)),
                dma((EXPERTS,)),
                dma((far, EXPERTS)),
                dma((far, EXPERTS)),
                dma((chips, EXPERTS)),
                dma((chips, EXPERTS)),
                dma((n_col,)),
                dma((n_col,)),
                dma((far, n_col)),
                dma((far, n_col)),
                dma((EXPERTS, n_col)),
                dma((EXPERTS, n_col)),
                dma((len(small),)),
            ],
            compiler_params=pltpu.CompilerParams(
                collective_id=0, has_side_effects=True, vmem_limit_bytes=61 * 1024 * 1024
            ),
        )(
            *small,
            input_weight,
            branch_weight,
            output_weight,
            expert_gate,
            expert_up,
            expert_down,
        )
        layer_out, new_hidden, new_inputs = pl.pallas_call(
            write_out,
            out_shape=(
                jax.ShapeDtypeStruct((seq, model), bf16),
                jax.ShapeDtypeStruct((seq, rnn), f32),
                jax.ShapeDtypeStruct(recent.shape, bf16),
            ),
            in_specs=[vmem] * 4,
            out_specs=(vmem, vmem, vmem),
            compiler_params=pltpu.CompilerParams(vmem_limit_bytes=4 * 1024 * 1024),
        )(layer_out, new_hidden, branch_x, recent)
        return (layer_out, new_hidden, jnp.transpose(new_inputs, (1, 0, 2)))

    placed = (
        P("ep", None),
        P("ep", None),
        P("ep", None, None),
        P("ep", None),
    ) + (P(),) * 10 + (P(None, "ep"), P(None, "ep"), P("ep", None))
    return jax.shard_map(
        local,
        mesh=mesh,
        in_specs=placed,
        out_specs=(P("ep", None), P("ep", None), P("ep", None, None)),
        check_vma=False,
    )
```
